32 devices in a mesh: sp: 4 (over z), fs: 4 (over y, x), tp: 2 (over core).
Axes of the slice: x: 2, y: 2, z: 4, core: 2. Of those that a mesh axis runs over, the one named last changes fastest.
Arguments:
- tokens: bfloat16 [4, 4096, 2048], P('fs', ('sp', 'tp')), may hold values from -6 to 6
- input_norm_gain: float32 [2048], replicated, may hold values from 0.1 to 1.9
- earlier_gate: bfloat16 [2048, 1024], P(('sp', 'fs'), 'tp'), may hold values from -0.125 to 0.125
- later_gate: bfloat16 [2048, 1024], P(('sp', 'fs'), 'tp'), may hold values from -0.125 to 0.125
- convolution_input: bfloat16 [2048, 1024], P(('sp', 'fs'), 'tp'), may hold values from -0.125 to 0.125
- convolution_taps: float32 [3, 1024], P(None, 'tp'), may hold values from -3 to 3
- receptance: bfloat16 [2048, 1024], P(('sp', 'fs'), 'tp'), may hold values from -0.125 to 0.125
- key_matrix: bfloat16 [2048, 1024], P(('sp', 'fs'), 'tp'), may hold values from -0.125 to 0.125
- value_matrix: bfloat16 [2048, 1024], P(('sp', 'fs'), 'tp'), may hold values from -0.125 to 0.125
- decay_matrix: bfloat16 [2048, 1024], P(('sp', 'fs'), 'tp'), may hold values from -0.125 to 0.125
- rate_matrix: bfloat16 [2048, 1024], P(('sp', 'fs'), 'tp'), may hold values from -0.125 to 0.125
- decay_floor: float32 [1024], P('tp'), may hold values from -16 to -3.4
- rate_offset: float32 [1024], P('tp'), may hold values from -7.5 to 1
- decay_spike: float32 [4, 4096, 1024], P('fs', 'sp', 'tp'), may hold values from -1.3 to 0
- initial_state: float32 [4, 16, 64, 64], P('fs', 'tp'), may hold values from -384 to 384
- head_norm_gain: float32 [1024], P('tp'), may hold values from 0.1 to 1.9
- convolution_output: bfloat16 [1024, 2048], P('tp', ('sp', 'fs')), may hold values from -0.125 to 0.125
- state_heads_output: bfloat16 [1024, 2048], P('tp', ('sp', 'fs')), may hold values from -0.125 to 0.125
Outputs:
- mixed: bfloat16 [4, 4096, 2048], P('fs', ('sp', 'tp'))
The draws below stay inside these ranges and needn't reach their ends.
All inputs are finite; a program needn't handle non-finite values.
Results may differ from the reference program's by a relative error of at most 0.02.
Values may be sent and summed in bfloat16 or wider, within the bound.
A program may use at most 128 MiB of HBM per device.

```python
import math
import jax
import jax.numpy as jnp
from jax import lax

D = 2048
HEAD_COUNT = 16
HEAD_WIDTH = 64
KERNEL = 3
TOK_DEV = 1024
SEQUENCE_LENGTH = 4096
SEQS = 4
N_TP = 2


def speed_mask(key, slow_count):
    order = jax.random.permutation(jax.random.fold_in(key, 101), HEAD_COUNT)
    return jnp.repeat(order < slow_count, HEAD_WIDTH)


def draw_decay_floor(key, part):
    slow_count = HEAD_COUNT // 2
    slow_channels = speed_mask(key, slow_count)
    jitter = jax.random.uniform(jax.random.fold_in(key, 102), (HEAD_COUNT * HEAD_WIDTH,), jnp.float32, -0.5, 0.5)
    return jnp.where(slow_channels, math.log(0.1 / SEQUENCE_LENGTH), math.log(0.02)) + jitter


def draw_rate_offset(key, part):
    slow_count = HEAD_COUNT // 2
    slow_channels = speed_mask(key, slow_count)
    slow_values = -7.0 + jax.random.uniform(jax.random.fold_in(key, 103), (HEAD_COUNT * HEAD_WIDTH,), jnp.float32, -0.5, 0.5)
    fast_values = jax.random.uniform(jax.random.fold_in(key, 104), (HEAD_COUNT * HEAD_WIDTH,), jnp.float32, -1.0, 1.0)
    return jnp.where(slow_channels, slow_values, fast_values)


def draw_decay_spike(key, part):
    segments = SEQUENCE_LENGTH // TOK_DEV
    drift = jnp.exp(jax.random.uniform(jax.random.fold_in(key, 105), (SEQS, segments, HEAD_COUNT), jnp.float32, math.log(0.1), math.log(0.6)))
    layer_depth = jax.random.uniform(jax.random.fold_in(key, 107), (SEQS, 2, HEAD_COUNT), jnp.float32, 0.22, 0.6)
    wander_rows = jnp.repeat(-drift / SEQUENCE_LENGTH, TOK_DEV, axis=1)
    spots = jax.random.randint(jax.random.fold_in(key, 106), (SEQS, 2, HEAD_COUNT), 0, SEQUENCE_LENGTH)
    positions = jnp.arange(SEQUENCE_LENGTH, dtype=jnp.int32)[None, :, None, None]
    matches = positions == spots[:, None, :, :]
    spikes = -jnp.sum(jnp.where(matches, layer_depth[:, None, :, :], 0.0), axis=2)
    return jnp.repeat(wander_rows + spikes, HEAD_WIDTH, axis=2).astype(jnp.float32)


def level_of(key, dims, split, smallest, high):
    def one(axis_at, blocks):
        draws = jax.random.uniform(jax.random.fold_in(jax.random.fold_in(key, 6), axis_at), (blocks,), jnp.float32, smallest / len(split), high / len(split))
        return jnp.repeat(jnp.exp(draws), dims[axis_at] // blocks).reshape((-1,) + (1,) * (len(dims) - axis_at - 1))

    factor_of = one(*split[0])
    for cut in split[1:]:
        factor_of = factor_of * one(*cut)
    return factor_of


def bell_draw(key, dims, width, limit, split=(), held_as=jnp.bfloat16):
    loudness = level_of(key, dims, split, -0.22, 0.18) if split else 1.0
    values = jax.random.normal(key, dims, jnp.float32) * width * loudness
    return jnp.minimum(jnp.maximum(values, -limit), limit).astype(held_as)


def setup_inputs(seed: int = 0) -> dict:
    key_of = jax.random.split(jax.random.key(seed), 19)
    return {
        "tokens": bell_draw(key_of[0], (SEQS, SEQUENCE_LENGTH, D), 1.0, 6.0, ((0, 4), (1, 8))),
        "input_norm_gain": jnp.clip(1.0 + 0.18 * jax.random.normal(key_of[1], (D,), jnp.float32), 0.1, 1.9),
        "earlier_gate": bell_draw(key_of[2], (D, HEAD_COUNT * HEAD_WIDTH), D ** -0.5, 0.125, ((0, 16), (1, 2))),
        "later_gate": bell_draw(key_of[3], (D, HEAD_COUNT * HEAD_WIDTH), D ** -0.5, 0.125, ((0, 16), (1, 2))),
        "convolution_input": bell_draw(key_of[4], (D, HEAD_COUNT * HEAD_WIDTH), D ** -0.5, 0.125, ((0, 16), (1, 2))),
        "convolution_taps": bell_draw(key_of[5], (KERNEL, HEAD_COUNT * HEAD_WIDTH), 0.5, 3.0, ((1, 2),), jnp.float32),
        "receptance": bell_draw(key_of[6], (D, HEAD_COUNT * HEAD_WIDTH), D ** -0.5, 0.125, ((0, 16), (1, 2))),
        "key_matrix": bell_draw(key_of[7], (D, HEAD_COUNT * HEAD_WIDTH), D ** -0.5, 0.125, ((0, 16), (1, 2))),
        "value_matrix": bell_draw(key_of[8], (D, HEAD_COUNT * HEAD_WIDTH), D ** -0.5, 0.125, ((0, 16), (1, 2))),
        "decay_matrix": bell_draw(key_of[9], (D, HEAD_COUNT * HEAD_WIDTH), D ** -0.5, 0.125, ((0, 16), (1, 2))),
        "rate_matrix": bell_draw(key_of[10], (D, HEAD_COUNT * HEAD_WIDTH), D ** -0.5, 0.125, ((0, 16), (1, 2))),
        "decay_floor": draw_decay_floor(jax.random.fold_in(key_of[18], 71), 0),
        "rate_offset": draw_rate_offset(jax.random.fold_in(key_of[18], 71), 0),
        "decay_spike": draw_decay_spike(jax.random.fold_in(key_of[18], 71), 0),
        "initial_state": bell_draw(key_of[14], (SEQS, HEAD_COUNT, HEAD_WIDTH, HEAD_WIDTH), (SEQUENCE_LENGTH ** 0.5), 384.0, ((0, 4), (1, 2)), jnp.float32),
        "head_norm_gain": jnp.clip(1.0 + 0.18 * jax.random.normal(key_of[15], (HEAD_COUNT * HEAD_WIDTH,), jnp.float32), 0.1, 1.9),
        "convolution_output": bell_draw(key_of[16], (HEAD_COUNT * HEAD_WIDTH, D), (2 * HEAD_COUNT * HEAD_WIDTH) ** -0.5, 0.125, ((0, 2), (1, 16))),
        "state_heads_output": bell_draw(key_of[17], (HEAD_COUNT * HEAD_WIDTH, D), (2 * HEAD_COUNT * HEAD_WIDTH) ** -0.5, 0.125, ((0, 2), (1, 16))),
    }


norm_eps = 1e-06
key_eps = 1e-06
highest = lax.Precision.HIGHEST

def rms_rows(activations, gain_vector):
    values = activations.astype(jnp.float32)
    inv_scale = lax.rsqrt(lax.optimization_barrier(jnp.mean(values * values, axis=-1, keepdims=True)) + norm_eps)
    return (values * inv_scale * gain_vector).astype(jnp.bfloat16)

def project(activations, weight):
    return jnp.dot(activations, weight, preferred_element_type=jnp.float32).astype(jnp.bfloat16)

def recur(state, inputs):
    queries, key_rows, value_rows, unit_keys, beta_rows, log_rows = inputs
    removed = jnp.einsum('hvk,hk->hv', state, unit_keys, precision=highest)
    state = state * jnp.exp(log_rows)[:, None, :] - removed[:, :, None] * beta_rows[:, None, :] + value_rows[:, :, None] * key_rows[:, None, :]
    return (state, jnp.einsum('hvk,hk->hv', state, queries, precision=highest))

def single_sequence(token_sequence, spike_rows, opening_state, weight_set):
    input_norm_gain, earlier_gate, later_gate, convolution_input, convolution_taps, receptance, key_matrix, value_matrix, decay_matrix, rate_matrix, decay_floor, rate_offset, head_norm_gain, convolution_output, state_heads_output = weight_set
    normed = rms_rows(token_sequence, input_norm_gain)
    product = project(normed, earlier_gate).astype(jnp.float32) * project(normed, convolution_input).astype(jnp.float32)
    padded = jnp.concatenate([jnp.zeros((KERNEL - 1, product.shape[1]), jnp.float32), product], axis=0)
    filtered = jnp.zeros_like(product)
    for offset in range(KERNEL):
        filtered = filtered + convolution_taps[offset] * padded[offset:offset + SEQUENCE_LENGTH]
    conv_mixed = (project(normed, later_gate).astype(jnp.float32) * filtered).astype(jnp.bfloat16)

    def by_heads(array):
        return array.astype(jnp.float32).reshape(SEQUENCE_LENGTH, HEAD_COUNT, HEAD_WIDTH)
    queries = by_heads(project(normed, receptance))
    key_rows = by_heads(project(normed, key_matrix))
    value_rows = by_heads(project(normed, value_matrix))
    logarithm_decay = -jnp.exp(decay_floor.reshape(HEAD_COUNT, HEAD_WIDTH) + jnp.tanh(by_heads(project(normed, decay_matrix))))
    logarithm_decay = logarithm_decay + spike_rows.reshape(SEQUENCE_LENGTH, HEAD_COUNT, HEAD_WIDTH)
    learn_rate = jax.nn.sigmoid(rate_offset.reshape(HEAD_COUNT, HEAD_WIDTH) + by_heads(project(normed, rate_matrix)))
    unit_keys = key_rows * lax.rsqrt(lax.optimization_barrier(jnp.sum(key_rows * key_rows, axis=-1, keepdims=True)) + key_eps)
    beta_rows = learn_rate * unit_keys
    final_state, reads = lax.scan(recur, opening_state, (queries, key_rows, value_rows, unit_keys, beta_rows, logarithm_decay))
    centered = reads - lax.optimization_barrier(jnp.mean(reads, axis=-1, keepdims=True))
    variance = lax.optimization_barrier(jnp.mean(centered * centered, axis=-1, keepdims=True))
    state_mixed = centered * lax.rsqrt(variance + HEAD_WIDTH * 1e-05) * head_norm_gain.reshape(HEAD_COUNT, HEAD_WIDTH)
    state_mixed = state_mixed.reshape(SEQUENCE_LENGTH, HEAD_COUNT * HEAD_WIDTH).astype(jnp.bfloat16)
    group_width = HEAD_COUNT * HEAD_WIDTH // N_TP
    summed = jnp.zeros((SEQUENCE_LENGTH, D), jnp.float32)
    for member in range(N_TP):
        column_start = member * group_width
        column_end = column_start + group_width
        partial_value = jnp.dot(conv_mixed[:, column_start:column_end], convolution_output[column_start:column_end], preferred_element_type=jnp.float32)
        partial_value = partial_value + jnp.dot(state_mixed[:, column_start:column_end], state_heads_output[column_start:column_end], preferred_element_type=jnp.float32)
        summed = summed + lax.optimization_barrier(partial_value.astype(jnp.bfloat16)).astype(jnp.float32)
    return summed.astype(jnp.bfloat16)

def reference(tokens, input_norm_gain, earlier_gate, later_gate, convolution_input, convolution_taps, receptance, key_matrix, value_matrix, decay_matrix, rate_matrix, decay_floor, rate_offset, decay_spike, initial_state, head_norm_gain, convolution_output, state_heads_output):
    weight_set = (input_norm_gain, earlier_gate, later_gate, convolution_input, convolution_taps, receptance, key_matrix, value_matrix, decay_matrix, rate_matrix, decay_floor, rate_offset, head_norm_gain, convolution_output, state_heads_output)

    def apply_single(inputs):
        return single_sequence(inputs[0], inputs[1], inputs[2], weight_set)
    return lax.map(apply_single, (tokens, decay_spike, initial_state))
```

```python
import jax
import jax.numpy as jnp
from jax import lax
from jax.experimental import pallas as pl
from jax.experimental.pallas import tpu as pltpu
from jax.sharding import PartitionSpec as P

HEAD_WIDTH = 64
BLOCK = 64


norm_eps = 1e-06
key_eps = 1e-06
highest = lax.Precision.HIGHEST


def passed_along(block, axis, distance):
    devices = range(lax.axis_size(axis))
    route = [(i - distance, i) for i in devices if i - distance in devices]
    return lax.ppermute(block, axis, route)


def rms_rows(activations, gain_vector):
    values = activations.astype(jnp.float32)
    inv_scale = lax.rsqrt(jnp.mean(values * values, axis=-1, keepdims=True) + norm_eps)
    return (values * inv_scale * gain_vector).astype(jnp.bfloat16)


def project(activations, weight):
    return jnp.dot(activations, weight, preferred_element_type=jnp.float32).astype(jnp.bfloat16)


def conv_branch(pre_values, post_values, conv_values, convolution_taps):
    product = pre_values.astype(jnp.float32) * conv_values.astype(jnp.float32)
    reach_rows = convolution_taps.shape[0] - 1
    sequence_rows = product.shape[0]
    edge_rows = passed_along(product[sequence_rows - reach_rows :], "sp", 1)
    padded = jnp.concatenate([edge_rows, product], axis=0)
    filtered = convolution_taps[0] * padded[0:sequence_rows]
    for offset in range(1, convolution_taps.shape[0]):
        filtered = filtered + convolution_taps[offset] * padded[offset : offset + sequence_rows]
    return (post_values.astype(jnp.float32) * filtered).astype(jnp.bfloat16)


def dot_bf16(left, right, contract):
    return lax.dot_general(
        left.astype(jnp.bfloat16),
        right.astype(jnp.bfloat16),
        (contract, ((), ())),
        preferred_element_type=jnp.float32,
    )


ROWS = ((1,), (0,))
TRANSPOSED_RIGHT = ((1,), (1,))
TRANSPOSED_LEFT = ((0,), (0,))


def split_dot(exact, wide, contract, left_exact):
    total = None
    rest = wide
    for _ in range(3):
        part = rest.astype(jnp.bfloat16)
        rest = rest - part.astype(jnp.float32)
        piece = (
            dot_bf16(exact, part, contract) if left_exact else dot_bf16(part, exact, contract)
        )
        total = piece if total is None else total + piece
    return total


def unit_inverse(lower, row, col, size):
    inverse = jnp.where(row == col, 1.0, 0.0) - jnp.where(
        ((row ^ col) == 1) & (row > col), lower, 0.0
    )
    width = 2
    while width < size:
        cross = ((row // (2 * width)) == (col // (2 * width))) & (
            (row // width) > (col // width)
        )
        step = dot_bf16(jnp.where(cross, lower, 0.0), inverse, ROWS)
        inverse = inverse - dot_bf16(inverse, step, ROWS)
        width *= 2
    return inverse


def delta_kernel(proj_ref, spike_ref, floor_ref, offset_ref, reads_ref, maps_ref, ending_ref, state):
    chunk = pl.program_id(0)
    channels = floor_ref.shape[1]
    span = spike_ref.shape[0]
    lanes = 2 * HEAD_WIDTH
    groups = channels // lanes

    @pl.when(chunk == 0)
    def _():
        row = lax.broadcasted_iota(jnp.int32, (2 * lanes, lanes), 0)
        col = lax.broadcasted_iota(jnp.int32, (2 * lanes, lanes), 1)
        start = jnp.where(row - lanes == col, 1.0, 0.0)
        for group in range(groups):
            state[group] = start

    def part(index):
        return proj_ref[:, index * channels : (index + 1) * channels].astype(jnp.float32)

    queries, keys, values, decay_pre, rate_pre = [part(i) for i in range(5)]
    log_decay = -jnp.exp(floor_ref[...] + jnp.tanh(decay_pre)) + spike_ref[...]
    rate = jax.nn.sigmoid(offset_ref[...] + rate_pre)
    tri = lax.broadcasted_iota(jnp.int32, (span, span), 0) >= lax.broadcasted_iota(
        jnp.int32, (span, span), 1
    )
    cumulative = split_dot(jnp.where(tri, 1.0, 0.0), log_decay, ROWS, True)
    previous = cumulative - log_decay
    middle = cumulative[span // 2 : span // 2 + 1]
    closing = cumulative[span - 1 : span]
    square = lax.broadcasted_iota(jnp.int32, (lanes, lanes), 0)
    across = lax.broadcasted_iota(jnp.int32, (lanes, lanes), 1)
    same_head = jnp.where((square // HEAD_WIDTH) == (across // HEAD_WIDTH), 1.0, 0.0)
    first_lanes = lax.broadcasted_iota(jnp.int32, (span, lanes), 1) < HEAD_WIDTH

    def by_head(array):
        return jnp.concatenate(
            [jnp.where(first_lanes, array, 0.0), jnp.where(first_lanes, 0.0, array)], axis=0
        ).astype(jnp.bfloat16)

    grow = jnp.exp(middle - cumulative)
    shrink_previous = jnp.exp(previous - middle)
    shrink = jnp.exp(cumulative - middle)
    from_previous = jnp.exp(previous)
    from_current = jnp.exp(cumulative)
    tail = jnp.exp(closing - cumulative)
    whole = jnp.exp(closing)
    strict = square > across
    inclusive = square >= across
    for group in range(groups):
        cols = slice(group * lanes, (group + 1) * lanes)
        key = keys[:, cols]
        query = queries[:, cols]
        square_sum = split_dot(same_head, key * key, ROWS, False)
        unit = key * lax.rsqrt(square_sum + key_eps)
        beta = rate[:, cols] * unit
        value = by_head(values[:, cols])
        asks = jnp.concatenate(
            [by_head(unit * shrink_previous[:, cols]), by_head(query * shrink[:, cols])], axis=0
        )
        gives = jnp.concatenate(
            [by_head(key * grow[:, cols]), by_head(beta * grow[:, cols])], axis=0
        )
        grams = dot_bf16(asks, gives, TRANSPOSED_RIGHT)
        key_ask = jnp.where(strict, grams[:lanes, :lanes], 0.0)
        beta_ask = jnp.where(strict, grams[:lanes, lanes:], 0.0)
        key_read = jnp.where(inclusive, grams[lanes:, :lanes], 0.0)
        beta_read = jnp.where(inclusive, grams[lanes:, lanes:], 0.0)
        inverse = unit_inverse(beta_ask, square, across, span)
        carried = state[group]
        openers = jnp.concatenate(
            [by_head(unit * from_previous[:, cols]), by_head(query * from_current[:, cols])],
            axis=0,
        )
        opened = dot_bf16(openers, carried, TRANSPOSED_RIGHT)
        inner = dot_bf16(jnp.concatenate([key_ask, key_read], axis=0), value, ROWS)
        right_side = jnp.concatenate(
            [opened[:lanes, :lanes] + inner[:lanes], opened[:lanes, lanes:]], axis=1
        )
        removed = dot_bf16(inverse, right_side, ROWS)
        taken = dot_bf16(beta_read, removed, ROWS)
        out_source = opened[lanes:, :lanes] + inner[lanes:] - taken[:, :lanes]
        out_map = opened[lanes:, lanes:] - taken[:, lanes:]
        reads_ref[:, cols] = out_source[:span] + out_source[span:]
        maps_ref[:, cols] = (out_map[:span] + out_map[span:]).astype(maps_ref.dtype)
        tails = jnp.concatenate(
            [by_head(key * tail[:, cols]), by_head(beta * tail[:, cols])], axis=0
        )
        lefts = jnp.concatenate(
            [
                jnp.concatenate([value, jnp.zeros_like(value)], axis=1),
                (-removed).astype(jnp.bfloat16),
            ],
            axis=0,
        )
        carried = carried * whole[:, cols] + dot_bf16(lefts, tails, TRANSPOSED_LEFT)
        state[group] = carried

    @pl.when(chunk == pl.num_programs(0) - 1)
    def _():
        ending_ref[...] = state[...]


def delta_mix(projected, spike, floor, offset):
    rows, channels = spike.shape
    lanes = 2 * HEAD_WIDTH
    groups = channels // lanes
    wide = projected.shape[1]
    return pl.pallas_call(
        delta_kernel,
        grid=(rows // BLOCK,),
        in_specs=[
            pl.BlockSpec((BLOCK, wide), lambda i: (i, 0)),
            pl.BlockSpec((BLOCK, channels), lambda i: (i, 0)),
            pl.BlockSpec((1, channels), lambda i: (0, 0)),
            pl.BlockSpec((1, channels), lambda i: (0, 0)),
        ],
        out_specs=[
            pl.BlockSpec((BLOCK, channels), lambda i: (i, 0)),
            pl.BlockSpec((BLOCK, channels), lambda i: (i, 0)),
            pl.BlockSpec((groups, 2 * lanes, lanes), lambda i: (0, 0, 0)),
        ],
        out_shape=[
            jax.ShapeDtypeStruct((rows, channels), jnp.float32),
            jax.ShapeDtypeStruct((rows, channels), jnp.bfloat16),
            jax.ShapeDtypeStruct((groups, 2 * lanes, lanes), jnp.float32),
        ],
        scratch_shapes=[pltpu.VMEM((groups, 2 * lanes, lanes), jnp.float32)],
        cost_estimate=pl.CostEstimate(
            flops=40 * rows * channels * lanes, bytes_accessed=20 * rows * channels, transcendentals=0
        ),
    )(projected, spike, floor.reshape(1, channels), offset.reshape(1, channels))


def apart(pair_blocks):
    groups = pair_blocks.shape[0]
    blocks = pair_blocks.reshape(groups, 2, HEAD_WIDTH, 2, HEAD_WIDTH)
    kept = jnp.stack([blocks[:, 0, :, 0], blocks[:, 1, :, 1]], axis=1)
    return kept.reshape(2 * groups, HEAD_WIDTH, HEAD_WIDTH)


def paired(heads):
    groups = heads.shape[0] // 2
    pairs = heads.reshape(groups, 2, HEAD_WIDTH, HEAD_WIDTH)
    zeros = jnp.zeros_like(pairs[:, 0])
    return jnp.concatenate(
        [
            jnp.concatenate([pairs[:, 0], zeros], axis=2),
            jnp.concatenate([zeros, pairs[:, 1]], axis=2),
        ],
        axis=1,
    )


def on_device(
    tokens,
    input_norm_gain,
    earlier_gate,
    later_gate,
    convolution_input,
    convolution_taps,
    receptance,
    key_matrix,
    value_matrix,
    decay_matrix,
    rate_matrix,
    decay_floor,
    rate_offset,
    decay_spike,
    initial_state,
    head_norm_gain,
    convolution_output,
    state_heads_output,
):
    normed = rms_rows(tokens[0], input_norm_gain)
    channels = earlier_gate.shape[1]
    state_weights = jnp.concatenate(
        [receptance, key_matrix, value_matrix, decay_matrix, rate_matrix], axis=1
    )
    conv_weights = jnp.concatenate([earlier_gate, later_gate, convolution_input], axis=1)
    piece = lax.all_gather(normed, "tp", axis=0, tiled=True)
    projected = project(piece, lax.all_gather(state_weights, ("sp", "fs"), axis=0, tiled=True))
    sequence_rows = projected.shape[0]
    present_heads = channels // HEAD_WIDTH
    source_reads, map_reads, ending = delta_mix(projected, decay_spike[0], decay_floor, rate_offset)
    conv_projected = project(
        piece, lax.all_gather(conv_weights, ("sp", "fs"), axis=0, tiled=True)
    )
    pieces = jnp.split(conv_projected, 3, axis=1)
    conv_mixed = conv_branch(pieces[0], pieces[1], pieces[2], convolution_taps)
    lanes = 2 * HEAD_WIDTH
    carry_source = apart(ending[:, :lanes])
    carry_map = apart(ending[:, lanes:])
    first_state = initial_state[0]
    is_first = lax.axis_index("sp") == 0

    def relay_turn(turn, received):
        current = jnp.where(is_first, first_state, received)
        passed = jnp.einsum("hvj,hjk->hvk", current, carry_map, precision=highest) + carry_source
        return passed_along(passed.astype(jnp.bfloat16), "sp", 1).astype(passed.dtype)

    received = lax.fori_loop(0, lax.axis_size("sp") - 1, relay_turn, jnp.zeros_like(first_state))
    opening_state = jnp.where(is_first, first_state, received)
    groups = present_heads // 2
    reads = source_reads.reshape(sequence_rows, groups, lanes) + jnp.einsum(
        "tgj,gvj->tgv",
        map_reads.reshape(sequence_rows, groups, lanes),
        paired(opening_state).astype(jnp.bfloat16),
        preferred_element_type=jnp.float32,
    )
    reads = reads.reshape(sequence_rows, present_heads, HEAD_WIDTH)
    centered = reads - jnp.mean(reads, axis=-1, keepdims=True)
    variance = jnp.mean(centered * centered, axis=-1, keepdims=True)
    state_mixed = (
        centered
        * lax.rsqrt(variance + HEAD_WIDTH * 1e-05)
        * head_norm_gain.reshape(present_heads, HEAD_WIDTH)
    )
    state_mixed = state_mixed.reshape(sequence_rows, channels).astype(jnp.bfloat16)
    conv_whole, state_whole = (
        lax.all_gather(convolution_output, ("sp", "fs"), axis=1, tiled=True),
        lax.all_gather(state_heads_output, ("sp", "fs"), axis=1, tiled=True),
    )
    mixed = lax.psum_scatter(
        (
            jnp.dot(conv_mixed, conv_whole, preferred_element_type=jnp.float32)
            + jnp.dot(state_mixed, state_whole, preferred_element_type=jnp.float32)
        ).astype(jnp.bfloat16),
        "tp",
        scatter_dimension=0,
        tiled=True,
    )
    return mixed[None]


def solution(mesh):
    placed = (
        P("fs", ("sp", "tp"), None),
        P(),
        P(("sp", "fs"), "tp"),
        P(("sp", "fs"), "tp"),
        P(("sp", "fs"), "tp"),
        P(None, "tp"),
        P(("sp", "fs"), "tp"),
        P(("sp", "fs"), "tp"),
        P(("sp", "fs"), "tp"),
        P(("sp", "fs"), "tp"),
        P(("sp", "fs"), "tp"),
        P("tp"),
        P("tp"),
        P("fs", "sp", "tp"),
        P("fs", "tp", None, None),
        P("tp"),
        P("tp", ("sp", "fs")),
        P("tp", ("sp", "fs")),
    )
    return jax.shard_map(
        on_device,
        mesh=mesh,
        in_specs=placed,
        out_specs=P("fs", ("sp", "tp"), None),
        check_vma=False,
    )
```

```python
import jax
import jax.numpy as jnp
from jax import lax
from jax.experimental import pallas as pl
from jax.experimental.pallas import tpu as pltpu
from jax.sharding import PartitionSpec as P

HEAD_WIDTH = 64
BLOCK = 64
STEP_BLOCKS = 2


norm_eps = 1e-06
key_eps = 1e-06
highest = lax.Precision.HIGHEST


def passed_along(block, axis, distance):
    devices = range(lax.axis_size(axis))
    route = [(i - distance, i) for i in devices if i - distance in devices]
    return lax.ppermute(block, axis, route)


def rms_rows(activations, gain_vector):
    values = activations.astype(jnp.float32)
    inv_scale = lax.rsqrt(jnp.mean(values * values, axis=-1, keepdims=True) + norm_eps)
    return (values * inv_scale * gain_vector).astype(jnp.bfloat16)


def project(activations, weight):
    return jnp.dot(activations, weight, preferred_element_type=jnp.float32).astype(jnp.bfloat16)


def conv_branch(pre_values, post_values, conv_values, convolution_taps):
    product = pre_values.astype(jnp.float32) * conv_values.astype(jnp.float32)
    reach_rows = convolution_taps.shape[0] - 1
    sequence_rows = product.shape[0]
    edge_rows = passed_along(product[sequence_rows - reach_rows :], "sp", 1)
    padded = jnp.concatenate([edge_rows, product], axis=0)
    filtered = convolution_taps[0] * padded[0:sequence_rows]
    for offset in range(1, convolution_taps.shape[0]):
        filtered = filtered + convolution_taps[offset] * padded[offset : offset + sequence_rows]
    return (post_values.astype(jnp.float32) * filtered).astype(jnp.bfloat16)


def dot_bf16(left, right, contract):
    return lax.dot_general(
        left.astype(jnp.bfloat16),
        right.astype(jnp.bfloat16),
        (contract, ((), ())),
        preferred_element_type=jnp.float32,
    )


ROWS = ((1,), (0,))
TRANSPOSED_RIGHT = ((1,), (1,))
TRANSPOSED_LEFT = ((0,), (0,))


def split_dot(exact, wide, contract, left_exact):
    total = None
    rest = wide
    for _ in range(3):
        part = rest.astype(jnp.bfloat16)
        rest = rest - part.astype(jnp.float32)
        piece = (
            dot_bf16(exact, part, contract) if left_exact else dot_bf16(part, exact, contract)
        )
        total = piece if total is None else total + piece
    return total


def unit_inverses(lowers, row, col, size):
    odd = ((row ^ col) == 1) & (row > col)
    eye = jnp.where(row == col, 1.0, 0.0)
    inverses = [eye - jnp.where(odd, lower, 0.0) for lower in lowers]
    lowers = [lower.astype(jnp.bfloat16) for lower in lowers]
    width = 2
    while width < size:
        cross = ((row // (2 * width)) == (col // (2 * width))) & (
            (row // width) > (col // width)
        )
        nears = [inverse.astype(jnp.bfloat16) for inverse in inverses]
        steps = [
            dot_bf16(jnp.where(cross, lower, jnp.zeros_like(lower)), near, ROWS)
            for lower, near in zip(lowers, nears)
        ]
        turns = [dot_bf16(near, step, ROWS) for near, step in zip(nears, steps)]
        inverses = [inverse - turn for inverse, turn in zip(inverses, turns)]
        width *= 2
    return inverses


def delta_kernel(proj_ref, spike_ref, floor_ref, offset_ref, reads_ref, maps_ref, ending_ref, state):
    chunk = pl.program_id(0)
    channels = floor_ref.shape[1]
    span = spike_ref.shape[0]
    lanes = 2 * HEAD_WIDTH
    groups = channels // lanes

    @pl.when(chunk == 0)
    def _():
        row = lax.broadcasted_iota(jnp.int32, (2 * lanes, lanes), 0)
        col = lax.broadcasted_iota(jnp.int32, (2 * lanes, lanes), 1)
        start = jnp.where(row - lanes == col, 1.0, 0.0)
        for group in range(groups):
            state[group] = start

    spans = [slice(at, at + BLOCK) for at in range(0, span, BLOCK)]
    tri = lax.broadcasted_iota(jnp.int32, (BLOCK, BLOCK), 0) >= lax.broadcasted_iota(
        jnp.int32, (BLOCK, BLOCK), 1
    )
    tri = jnp.where(tri, 1.0, 0.0)
    square = lax.broadcasted_iota(jnp.int32, (lanes, lanes), 0)
    across = lax.broadcasted_iota(jnp.int32, (lanes, lanes), 1)
    same_head = jnp.where((square // HEAD_WIDTH) == (across // HEAD_WIDTH), 1.0, 0.0)
    first_lanes = lax.broadcasted_iota(jnp.int32, (BLOCK, lanes), 1) < HEAD_WIDTH
    strict = square > across
    inclusive = square >= across

    def by_head(array):
        array = array.astype(jnp.bfloat16)
        zeros = jnp.zeros_like(array)
        return jnp.concatenate(
            [jnp.where(first_lanes, array, zeros), jnp.where(first_lanes, zeros, array)], axis=0
        )

    def stacked(*arrays):
        return jnp.concatenate([by_head(array) for array in arrays], axis=0)

    work = [(at, group) for at in spans for group in range(groups)]

    def part(index, at, group):
        begin = index * channels + group * lanes
        return proj_ref[at, begin : begin + lanes].astype(jnp.float32)

    def column(ref, at, group):
        return ref[at, group * lanes : (group + 1) * lanes]

    asks, gives, openers, tails, values, wholes = [], [], [], [], [], []
    every = slice(0, 1)
    logs = [
        -jnp.exp(column(floor_ref, every, g) + jnp.tanh(part(3, at, g))) + column(spike_ref, at, g)
        for at, g in work
    ]
    sums = [split_dot(tri, log, ROWS, True) for log in logs]
    raw_keys = [part(1, at, g) for at, g in work]
    norms = [split_dot(same_head, key * key, ROWS, False) for key in raw_keys]
    for (at, g), log, cumulative, key, norm in zip(work, logs, sums, raw_keys, norms):
        query = part(0, at, g)
        unit = key * lax.rsqrt(norm + key_eps)
        beta = jax.nn.sigmoid(column(offset_ref, every, g) + part(4, at, g)) * unit
        previous = cumulative - log
        middle = cumulative[BLOCK // 2 : BLOCK // 2 + 1]
        closing = cumulative[BLOCK - 1 : BLOCK]
        grow = jnp.exp(middle - cumulative)
        tail = jnp.exp(closing - cumulative)
        asks.append(stacked(unit * jnp.exp(previous - middle), query * jnp.exp(cumulative - middle)))
        gives.append(stacked(key * grow, beta * grow))
        openers.append(stacked(unit * jnp.exp(previous), query * jnp.exp(cumulative)))
        tails.append(stacked(key * tail, beta * tail))
        values.append(by_head(part(2, at, g)))
        wholes.append(jnp.exp(closing))
    grams = [dot_bf16(ask, give, TRANSPOSED_RIGHT) for ask, give in zip(asks, gives)]
    inners = [
        dot_bf16(
            jnp.concatenate(
                [
                    jnp.where(strict, gram[:lanes, :lanes], 0.0),
                    jnp.where(inclusive, gram[lanes:, :lanes], 0.0),
                ],
                axis=0,
            ),
            value,
            ROWS,
        )
        for gram, value in zip(grams, values)
    ]
    beta_reads = [
        jnp.where(inclusive, gram[lanes:, lanes:], 0.0).astype(jnp.bfloat16) for gram in grams
    ]
    inverses = unit_inverses(
        [jnp.where(strict, gram[:lanes, lanes:], 0.0) for gram in grams], square, across, BLOCK
    )
    inverses = [inverse.astype(jnp.bfloat16) for inverse in inverses]
    for index, at in enumerate(spans):
        picks = range(index * groups, (index + 1) * groups)
        carried = [state[g] for g in range(groups)]
        opened = [dot_bf16(openers[i], carried[g], TRANSPOSED_RIGHT) for g, i in enumerate(picks)]
        rights = [
            jnp.concatenate(
                [opened[g][:lanes, :lanes] + inners[i][:lanes], opened[g][:lanes, lanes:]], axis=1
            )
            for g, i in enumerate(picks)
        ]
        removed = [
            dot_bf16(inverses[i], rights[g], ROWS).astype(jnp.bfloat16)
            for g, i in enumerate(picks)
        ]
        changes = [
            dot_bf16(
                jnp.concatenate(
                    [
                        jnp.concatenate([values[i], jnp.zeros_like(values[i])], axis=1),
                        -removed[g],
                    ],
                    axis=0,
                ),
                tails[i],
                TRANSPOSED_LEFT,
            )
            for g, i in enumerate(picks)
        ]
        taken = [dot_bf16(beta_reads[i], removed[g], ROWS) for g, i in enumerate(picks)]
        for g, i in enumerate(picks):
            state[g] = carried[g] * wholes[i] + changes[g]
            cols = slice(g * lanes, (g + 1) * lanes)
            out_source = opened[g][lanes:, :lanes] + inners[i][lanes:] - taken[g][:, :lanes]
            out_map = opened[g][lanes:, lanes:] - taken[g][:, lanes:]
            reads_ref[at, cols] = out_source[:BLOCK] + out_source[BLOCK:]
            maps_ref[at, cols] = (out_map[:BLOCK] + out_map[BLOCK:]).astype(maps_ref.dtype)

    @pl.when(chunk == pl.num_programs(0) - 1)
    def _():
        ending_ref[...] = state[...]


def delta_mix(projected, spike, floor, offset):
    rows, channels = spike.shape
    lanes = 2 * HEAD_WIDTH
    groups = channels // lanes
    wide = projected.shape[1]
    turn = STEP_BLOCKS * BLOCK
    return pl.pallas_call(
        delta_kernel,
        grid=(rows // turn,),
        in_specs=[
            pl.BlockSpec((turn, wide), lambda i: (i, 0)),
            pl.BlockSpec((turn, channels), lambda i: (i, 0)),
            pl.BlockSpec((1, channels), lambda i: (0, 0)),
            pl.BlockSpec((1, channels), lambda i: (0, 0)),
        ],
        out_specs=[
            pl.BlockSpec((turn, channels), lambda i: (i, 0)),
            pl.BlockSpec((turn, channels), lambda i: (i, 0)),
            pl.BlockSpec((groups, 2 * lanes, lanes), lambda i: (0, 0, 0)),
        ],
        out_shape=[
            jax.ShapeDtypeStruct((rows, channels), jnp.float32),
            jax.ShapeDtypeStruct((rows, channels), jnp.bfloat16),
            jax.ShapeDtypeStruct((groups, 2 * lanes, lanes), jnp.float32),
        ],
        scratch_shapes=[pltpu.VMEM((groups, 2 * lanes, lanes), jnp.float32)],
        cost_estimate=pl.CostEstimate(
            flops=40 * rows * channels * lanes, bytes_accessed=20 * rows * channels, transcendentals=0
        ),
    )(projected, spike, floor.reshape(1, channels), offset.reshape(1, channels))


def apart(pair_blocks):
    groups = pair_blocks.shape[0]
    blocks = pair_blocks.reshape(groups, 2, HEAD_WIDTH, 2, HEAD_WIDTH)
    kept = jnp.stack([blocks[:, 0, :, 0], blocks[:, 1, :, 1]], axis=1)
    return kept.reshape(2 * groups, HEAD_WIDTH, HEAD_WIDTH)


def paired(heads):
    groups = heads.shape[0] // 2
    pairs = heads.reshape(groups, 2, HEAD_WIDTH, HEAD_WIDTH)
    zeros = jnp.zeros_like(pairs[:, 0])
    return jnp.concatenate(
        [
            jnp.concatenate([pairs[:, 0], zeros], axis=2),
            jnp.concatenate([zeros, pairs[:, 1]], axis=2),
        ],
        axis=1,
    )


def on_device(
    tokens,
    input_norm_gain,
    earlier_gate,
    later_gate,
    convolution_input,
    convolution_taps,
    receptance,
    key_matrix,
    value_matrix,
    decay_matrix,
    rate_matrix,
    decay_floor,
    rate_offset,
    decay_spike,
    initial_state,
    head_norm_gain,
    convolution_output,
    state_heads_output,
):
    normed = rms_rows(tokens[0], input_norm_gain)
    channels = earlier_gate.shape[1]
    state_weights = jnp.concatenate(
        [receptance, key_matrix, value_matrix, decay_matrix, rate_matrix], axis=1
    )
    conv_weights = jnp.concatenate([earlier_gate, later_gate, convolution_input], axis=1)
    piece = lax.all_gather(normed, "tp", axis=0, tiled=True)
    state_whole = lax.all_gather(state_weights, ("sp", "fs"), axis=0, tiled=True)
    outgoing = jnp.concatenate([convolution_output, state_heads_output], axis=0)
    state_whole, conv_weights, outgoing = lax.optimization_barrier(
        (state_whole, conv_weights, outgoing)
    )
    projected = project(piece, state_whole)
    sequence_rows = projected.shape[0]
    present_heads = channels // HEAD_WIDTH
    source_reads, map_reads, ending = delta_mix(projected, decay_spike[0], decay_floor, rate_offset)
    conv_projected = project(
        piece, lax.all_gather(conv_weights, ("sp", "fs"), axis=0, tiled=True)
    )
    pieces = jnp.split(conv_projected, 3, axis=1)
    conv_mixed = conv_branch(pieces[0], pieces[1], pieces[2], convolution_taps)
    lanes = 2 * HEAD_WIDTH
    carry_source = apart(ending[:, :lanes])
    carry_map = apart(ending[:, lanes:])
    first_state = initial_state[0]
    is_first = lax.axis_index("sp") == 0

    def relay_turn(turn, received):
        current = jnp.where(is_first, first_state, received)
        passed = jnp.einsum("hvj,hjk->hvk", current, carry_map, precision=highest) + carry_source
        return passed_along(passed.astype(jnp.bfloat16), "sp", 1).astype(passed.dtype)

    received = lax.fori_loop(0, lax.axis_size("sp") - 1, relay_turn, jnp.zeros_like(first_state))
    opening_state = jnp.where(is_first, first_state, received)
    groups = present_heads // 2
    reads = source_reads.reshape(sequence_rows, groups, lanes) + jnp.einsum(
        "tgj,gvj->tgv",
        map_reads.reshape(sequence_rows, groups, lanes),
        paired(opening_state).astype(jnp.bfloat16),
        preferred_element_type=jnp.float32,
    )
    reads = reads.reshape(sequence_rows, present_heads, HEAD_WIDTH)
    centered = reads - jnp.mean(reads, axis=-1, keepdims=True)
    variance = jnp.mean(centered * centered, axis=-1, keepdims=True)
    state_mixed = (
        centered
        * lax.rsqrt(variance + HEAD_WIDTH * 1e-05)
        * head_norm_gain.reshape(present_heads, HEAD_WIDTH)
    )
    state_mixed = state_mixed.reshape(sequence_rows, channels).astype(jnp.bfloat16)
    out_whole = lax.all_gather(outgoing, ("sp", "fs"), axis=1, tiled=True)
    mixed = lax.psum_scatter(
        (
            jnp.dot(
                jnp.concatenate([conv_mixed, state_mixed], axis=1),
                out_whole,
                preferred_element_type=jnp.float32,
            )
        ).astype(jnp.bfloat16),
        "tp",
        scatter_dimension=0,
        tiled=True,
    )
    return mixed[None]


def solution(mesh):
    placed = (
        P("fs", ("sp", "tp"), None),
        P(),
        P(("sp", "fs"), "tp"),
        P(("sp", "fs"), "tp"),
        P(("sp", "fs"), "tp"),
        P(None, "tp"),
        P(("sp", "fs"), "tp"),
        P(("sp", "fs"), "tp"),
        P(("sp", "fs"), "tp"),
        P(("sp", "fs"), "tp"),
        P(("sp", "fs"), "tp"),
        P("tp"),
        P("tp"),
        P("fs", "sp", "tp"),
        P("fs", "tp", None, None),
        P("tp"),
        P("tp", ("sp", "fs")),
        P("tp", ("sp", "fs")),
    )
    return jax.shard_map(
        on_device,
        mesh=mesh,
        in_specs=placed,
        out_specs=P("fs", ("sp", "tp"), None),
        check_vma=False,
    )
```

```python
import jax
import jax.numpy as jnp
from jax import lax
from jax.experimental import pallas as pl
from jax.experimental.pallas import tpu as pltpu
from jax.sharding import PartitionSpec as P

HEAD_WIDTH = 64
BLOCK = 64
STEP_BLOCKS = 2


norm_eps = 1e-06
key_eps = 1e-06
highest = lax.Precision.HIGHEST


def passed_along(block, axis, distance):
    devices = range(lax.axis_size(axis))
    route = [(i - distance, i) for i in devices if i - distance in devices]
    return lax.ppermute(block, axis, route)


def rotated(block, axis, distance):
    count = lax.axis_size(axis)
    return lax.ppermute(block, axis, [(i, (i + distance) % count) for i in range(count)])


def permuted_columns(block, outer, inner):
    outer_count, inner_count = lax.axis_size(outer), lax.axis_size(inner)
    width = block.shape[1]
    column = [block] + [rotated(block, outer, d) for d in range(1, outer_count)]
    stack = jnp.stack(column)
    stacks = [stack] + [rotated(stack, inner, d) for d in range(1, inner_count)]
    whole = jnp.zeros((block.shape[0], outer_count * inner_count * width), block.dtype)
    for e in range(inner_count):
        inner_at = (lax.axis_index(inner) - e + inner_count) % inner_count
        for d in range(outer_count):
            outer_at = (lax.axis_index(outer) - d + outer_count) % outer_count
            start = (outer_at * inner_count + inner_at) * width
            whole = lax.dynamic_update_slice(whole, stacks[e][d], (0, start))
    return whole


def rms_rows(activations, gain_vector):
    values = activations.astype(jnp.float32)
    inv_scale = lax.rsqrt(jnp.mean(values * values, axis=-1, keepdims=True) + norm_eps)
    return (values * inv_scale * gain_vector).astype(jnp.bfloat16)


def project(activations, weight):
    return jnp.dot(activations, weight, preferred_element_type=jnp.float32).astype(jnp.bfloat16)


def conv_branch(pre_values, post_values, conv_values, convolution_taps):
    product = pre_values.astype(jnp.float32) * conv_values.astype(jnp.float32)
    reach_rows = convolution_taps.shape[0] - 1
    sequence_rows = product.shape[0]
    edge_rows = passed_along(product[sequence_rows - reach_rows :], "sp", 1)
    padded = jnp.concatenate([edge_rows, product], axis=0)
    filtered = convolution_taps[0] * padded[0:sequence_rows]
    for offset in range(1, convolution_taps.shape[0]):
        filtered = filtered + convolution_taps[offset] * padded[offset : offset + sequence_rows]
    return (post_values.astype(jnp.float32) * filtered).astype(jnp.bfloat16)


def dot_bf16(left, right, contract):
    return lax.dot_general(
        left.astype(jnp.bfloat16),
        right.astype(jnp.bfloat16),
        (contract, ((), ())),
        preferred_element_type=jnp.float32,
    )


ROWS = ((1,), (0,))
TRANSPOSED_RIGHT = ((1,), (1,))
TRANSPOSED_LEFT = ((0,), (0,))


def split_dot(exact, wide, contract, left_exact):
    total = None
    rest = wide
    for _ in range(3):
        part = rest.astype(jnp.bfloat16)
        rest = rest - part.astype(jnp.float32)
        piece = (
            dot_bf16(exact, part, contract) if left_exact else dot_bf16(part, exact, contract)
        )
        total = piece if total is None else total + piece
    return total


def unit_inverses(lowers, row, col, size):
    odd = ((row ^ col) == 1) & (row > col)
    eye = jnp.where(row == col, 1.0, 0.0)
    inverses = [eye - jnp.where(odd, lower, 0.0) for lower in lowers]
    lowers = [lower.astype(jnp.bfloat16) for lower in lowers]
    width = 2
    while width < size:
        cross = ((row // (2 * width)) == (col // (2 * width))) & (
            (row // width) > (col // width)
        )
        nears = [inverse.astype(jnp.bfloat16) for inverse in inverses]
        steps = [
            dot_bf16(jnp.where(cross, lower, jnp.zeros_like(lower)), near, ROWS)
            for lower, near in zip(lowers, nears)
        ]
        turns = [dot_bf16(near, step, ROWS) for near, step in zip(nears, steps)]
        inverses = [inverse - turn for inverse, turn in zip(inverses, turns)]
        width *= 2
    return inverses


def delta_kernel(proj_ref, spike_ref, floor_ref, offset_ref, reads_ref, maps_ref, ending_ref, state):
    chunk = pl.program_id(0)
    channels = floor_ref.shape[1]
    span = spike_ref.shape[0]
    lanes = 2 * HEAD_WIDTH
    groups = channels // lanes

    @pl.when(chunk == 0)
    def _():
        row = lax.broadcasted_iota(jnp.int32, (2 * lanes, lanes), 0)
        col = lax.broadcasted_iota(jnp.int32, (2 * lanes, lanes), 1)
        start = jnp.where(row - lanes == col, 1.0, 0.0)
        for group in range(groups):
            state[group] = start

    spans = [slice(at, at + BLOCK) for at in range(0, span, BLOCK)]
    tri = lax.broadcasted_iota(jnp.int32, (BLOCK, BLOCK), 0) >= lax.broadcasted_iota(
        jnp.int32, (BLOCK, BLOCK), 1
    )
    tri = jnp.where(tri, 1.0, 0.0)
    square = lax.broadcasted_iota(jnp.int32, (lanes, lanes), 0)
    across = lax.broadcasted_iota(jnp.int32, (lanes, lanes), 1)
    same_head = jnp.where((square // HEAD_WIDTH) == (across // HEAD_WIDTH), 1.0, 0.0)
    first_lanes = lax.broadcasted_iota(jnp.int32, (BLOCK, lanes), 1) < HEAD_WIDTH
    strict = square > across
    inclusive = square >= across

    def by_head(array):
        array = array.astype(jnp.bfloat16)
        zeros = jnp.zeros_like(array)
        return jnp.concatenate(
            [jnp.where(first_lanes, array, zeros), jnp.where(first_lanes, zeros, array)], axis=0
        )

    def stacked(*arrays):
        return jnp.concatenate([by_head(array) for array in arrays], axis=0)

    work = [(at, group) for at in spans for group in range(groups)]

    def part(index, at, group):
        begin = index * channels + group * lanes
        return proj_ref[at, begin : begin + lanes].astype(jnp.float32)

    def column(ref, at, group):
        return ref[at, group * lanes : (group + 1) * lanes]

    asks, gives, openers, tails, values, wholes = [], [], [], [], [], []
    every = slice(0, 1)
    logs = [
        -jnp.exp(column(floor_ref, every, g) + jnp.tanh(part(3, at, g))) + column(spike_ref, at, g)
        for at, g in work
    ]
    sums = [split_dot(tri, log, ROWS, True) for log in logs]
    raw_keys = [part(1, at, g) for at, g in work]
    norms = [split_dot(same_head, key * key, ROWS, False) for key in raw_keys]
    for (at, g), log, cumulative, key, norm in zip(work, logs, sums, raw_keys, norms):
        query = part(0, at, g)
        unit = key * lax.rsqrt(norm + key_eps)
        beta = jax.nn.sigmoid(column(offset_ref, every, g) + part(4, at, g)) * unit
        previous = cumulative - log
        middle = cumulative[BLOCK // 2 : BLOCK // 2 + 1]
        closing = cumulative[BLOCK - 1 : BLOCK]
        grow = jnp.exp(middle - cumulative)
        tail = jnp.exp(closing - cumulative)
        asks.append(stacked(unit * jnp.exp(previous - middle), query * jnp.exp(cumulative - middle)))
        gives.append(stacked(key * grow, beta * grow))
        openers.append(stacked(unit * jnp.exp(previous), query * jnp.exp(cumulative)))
        tails.append(stacked(key * tail, beta * tail))
        values.append(by_head(part(2, at, g)))
        wholes.append(jnp.exp(closing))
    grams = [dot_bf16(ask, give, TRANSPOSED_RIGHT) for ask, give in zip(asks, gives)]
    inners = [
        dot_bf16(
            jnp.concatenate(
                [
                    jnp.where(strict, gram[:lanes, :lanes], 0.0),
                    jnp.where(inclusive, gram[lanes:, :lanes], 0.0),
                ],
                axis=0,
            ),
            value,
            ROWS,
        )
        for gram, value in zip(grams, values)
    ]
    beta_reads = [
        jnp.where(inclusive, gram[lanes:, lanes:], 0.0).astype(jnp.bfloat16) for gram in grams
    ]
    inverses = unit_inverses(
        [jnp.where(strict, gram[:lanes, lanes:], 0.0) for gram in grams], square, across, BLOCK
    )
    inverses = [inverse.astype(jnp.bfloat16) for inverse in inverses]
    for index, at in enumerate(spans):
        picks = range(index * groups, (index + 1) * groups)
        carried = [state[g] for g in range(groups)]
        opened = [dot_bf16(openers[i], carried[g], TRANSPOSED_RIGHT) for g, i in enumerate(picks)]
        rights = [
            jnp.concatenate(
                [opened[g][:lanes, :lanes] + inners[i][:lanes], opened[g][:lanes, lanes:]], axis=1
            )
            for g, i in enumerate(picks)
        ]
        removed = [
            dot_bf16(inverses[i], rights[g], ROWS).astype(jnp.bfloat16)
            for g, i in enumerate(picks)
        ]
        changes = [
            dot_bf16(
                jnp.concatenate(
                    [
                        jnp.concatenate([values[i], jnp.zeros_like(values[i])], axis=1),
                        -removed[g],
                    ],
                    axis=0,
                ),
                tails[i],
                TRANSPOSED_LEFT,
            )
            for g, i in enumerate(picks)
        ]
        taken = [dot_bf16(beta_reads[i], removed[g], ROWS) for g, i in enumerate(picks)]
        for g, i in enumerate(picks):
            state[g] = carried[g] * wholes[i] + changes[g]
            cols = slice(g * lanes, (g + 1) * lanes)
            out_source = opened[g][lanes:, :lanes] + inners[i][lanes:] - taken[g][:, :lanes]
            out_map = opened[g][lanes:, lanes:] - taken[g][:, lanes:]
            reads_ref[at, cols] = out_source[:BLOCK] + out_source[BLOCK:]
            maps_ref[at, cols] = (out_map[:BLOCK] + out_map[BLOCK:]).astype(maps_ref.dtype)

    @pl.when(chunk == pl.num_programs(0) - 1)
    def _():
        ending_ref[...] = state[...]


def delta_mix(projected, spike, floor, offset):
    rows, channels = spike.shape
    lanes = 2 * HEAD_WIDTH
    groups = channels // lanes
    wide = projected.shape[1]
    turn = STEP_BLOCKS * BLOCK
    return pl.pallas_call(
        delta_kernel,
        grid=(rows // turn,),
        in_specs=[
            pl.BlockSpec((turn, wide), lambda i: (i, 0)),
            pl.BlockSpec((turn, channels), lambda i: (i, 0)),
            pl.BlockSpec((1, channels), lambda i: (0, 0)),
            pl.BlockSpec((1, channels), lambda i: (0, 0)),
        ],
        out_specs=[
            pl.BlockSpec((turn, channels), lambda i: (i, 0)),
            pl.BlockSpec((turn, channels), lambda i: (i, 0)),
            pl.BlockSpec((groups, 2 * lanes, lanes), lambda i: (0, 0, 0)),
        ],
        out_shape=[
            jax.ShapeDtypeStruct((rows, channels), jnp.float32),
            jax.ShapeDtypeStruct((rows, channels), jnp.bfloat16),
            jax.ShapeDtypeStruct((groups, 2 * lanes, lanes), jnp.float32),
        ],
        scratch_shapes=[pltpu.VMEM((groups, 2 * lanes, lanes), jnp.float32)],
        cost_estimate=pl.CostEstimate(
            flops=40 * rows * channels * lanes, bytes_accessed=20 * rows * channels, transcendentals=0
        ),
    )(projected, spike, floor.reshape(1, channels), offset.reshape(1, channels))


def apart(pair_blocks):
    groups = pair_blocks.shape[0]
    blocks = pair_blocks.reshape(groups, 2, HEAD_WIDTH, 2, HEAD_WIDTH)
    kept = jnp.stack([blocks[:, 0, :, 0], blocks[:, 1, :, 1]], axis=1)
    return kept.reshape(2 * groups, HEAD_WIDTH, HEAD_WIDTH)


def paired(heads):
    groups = heads.shape[0] // 2
    pairs = heads.reshape(groups, 2, HEAD_WIDTH, HEAD_WIDTH)
    zeros = jnp.zeros_like(pairs[:, 0])
    return jnp.concatenate(
        [
            jnp.concatenate([pairs[:, 0], zeros], axis=2),
            jnp.concatenate([zeros, pairs[:, 1]], axis=2),
        ],
        axis=1,
    )


def on_device(
    tokens,
    input_norm_gain,
    earlier_gate,
    later_gate,
    convolution_input,
    convolution_taps,
    receptance,
    key_matrix,
    value_matrix,
    decay_matrix,
    rate_matrix,
    decay_floor,
    rate_offset,
    decay_spike,
    initial_state,
    head_norm_gain,
    convolution_output,
    state_heads_output,
):
    normed = rms_rows(tokens[0], input_norm_gain)
    channels = earlier_gate.shape[1]
    state_weights = jnp.concatenate(
        [receptance, key_matrix, value_matrix, decay_matrix, rate_matrix], axis=1
    )
    conv_weights = jnp.concatenate([earlier_gate, later_gate, convolution_input], axis=1)
    piece = lax.all_gather(normed, "tp", axis=0, tiled=True)
    state_whole = lax.all_gather(state_weights, ("sp", "fs"), axis=0, tiled=True)
    outgoing = jnp.concatenate([convolution_output, state_heads_output], axis=0)
    state_whole, conv_weights, outgoing = lax.optimization_barrier(
        (state_whole, conv_weights, outgoing)
    )
    projected = project(piece, state_whole)
    sequence_rows = projected.shape[0]
    present_heads = channels // HEAD_WIDTH
    source_reads, map_reads, ending = delta_mix(projected, decay_spike[0], decay_floor, rate_offset)
    conv_projected = project(
        piece, lax.all_gather(conv_weights, ("sp", "fs"), axis=0, tiled=True)
    )
    pieces = jnp.split(conv_projected, 3, axis=1)
    conv_mixed = conv_branch(pieces[0], pieces[1], pieces[2], convolution_taps)
    lanes = 2 * HEAD_WIDTH
    carry_source = apart(ending[:, :lanes])
    carry_map = apart(ending[:, lanes:])
    first_state = initial_state[0]
    is_first = lax.axis_index("sp") == 0

    def relay_turn(turn, received):
        current = jnp.where(is_first, first_state, received)
        passed = jnp.einsum("hvj,hjk->hvk", current, carry_map, precision=highest) + carry_source
        return passed_along(passed.astype(jnp.bfloat16), "sp", 1).astype(passed.dtype)

    received = lax.fori_loop(0, lax.axis_size("sp") - 1, relay_turn, jnp.zeros_like(first_state))
    opening_state = jnp.where(is_first, first_state, received)
    groups = present_heads // 2
    reads = source_reads.reshape(sequence_rows, groups, lanes) + jnp.einsum(
        "tgj,gvj->tgv",
        map_reads.reshape(sequence_rows, groups, lanes),
        paired(opening_state).astype(jnp.bfloat16),
        preferred_element_type=jnp.float32,
    )
    reads = reads.reshape(sequence_rows, present_heads, HEAD_WIDTH)
    centered = reads - jnp.mean(reads, axis=-1, keepdims=True)
    variance = jnp.mean(centered * centered, axis=-1, keepdims=True)
    state_mixed = (
        centered
        * lax.rsqrt(variance + HEAD_WIDTH * 1e-05)
        * head_norm_gain.reshape(present_heads, HEAD_WIDTH)
    )
    state_mixed = state_mixed.reshape(sequence_rows, channels).astype(jnp.bfloat16)
    out_whole = permuted_columns(outgoing, "sp", "fs")
    mixed = lax.psum_scatter(
        (
            jnp.dot(
                jnp.concatenate([conv_mixed, state_mixed], axis=1),
                out_whole,
                preferred_element_type=jnp.float32,
            )
        ).astype(jnp.bfloat16),
        "tp",
        scatter_dimension=0,
        tiled=True,
    )
    return mixed[None]


def solution(mesh):
    placed = (
        P("fs", ("sp", "tp"), None),
        P(),
        P(("sp", "fs"), "tp"),
        P(("sp", "fs"), "tp"),
        P(("sp", "fs"), "tp"),
        P(None, "tp"),
        P(("sp", "fs"), "tp"),
        P(("sp", "fs"), "tp"),
        P(("sp", "fs"), "tp"),
        P(("sp", "fs"), "tp"),
        P(("sp", "fs"), "tp"),
        P("tp"),
        P("tp"),
        P("fs", "sp", "tp"),
        P("fs", "tp", None, None),
        P("tp"),
        P("tp", ("sp", "fs")),
        P("tp", ("sp", "fs")),
    )
    return jax.shard_map(
        on_device,
        mesh=mesh,
        in_specs=placed,
        out_specs=P("fs", ("sp", "tp"), None),
        check_vma=False,
    )
```
